768 devices in a mesh: rep: 3 (over z_hi), fs: 32 (over z_lo, y), tp: 8 (over x, core).
Axes of the slice: x: 4, y: 8, z: 12 (z_hi: 3, z_lo: 4; z = z_hi * 4 + z_lo), core: 2. Of those that a mesh axis runs over, the one named last changes fastest.
Arguments:
- tokens: bfloat16 [24576, 2048], P(('rep', 'fs')), may hold values from -6 to 6
- mix_gain: float32 [2048], replicated, may hold values from 0.1 to 1.9
- group_weight: float32 [512, 2048], P('fs', 'tp'), may hold values from -0.25 to 0.25
- group_scale: float32 [1, 2048], P(None, 'tp'), may hold values from 0.5 to 2
- mlp_gain: float32 [2048], replicated, may hold values from 0.1 to 1.9
- up_weight: float32 [2048, 8192], P('fs', 'tp'), may hold values from -0.125 to 0.125
- up_scale: float32 [1, 8192], P(None, 'tp'), may hold values from 0.5 to 2
- down_weight: float32 [8192, 2048], P('tp', 'fs'), may hold values from -0.0625 to 0.0625
- down_scale: float32 [1, 2048], replicated, may hold values from 0.5 to 2
Outputs:
- layer_out: bfloat16 [24576, 2048], P(('rep', 'fs'))
The draws below stay inside these ranges and needn't reach their ends.
All inputs are finite; a program needn't handle non-finite values.
Results may differ from the reference program's by a relative error of at most 0.013.
Values may be sent and summed in bfloat16 or wider, within the bound.
A program may use at most 64 MiB of HBM per device.

```python
import math
import jax
import jax.numpy as jnp
from jax import lax

D = 2048
FF = 8192
GROUPS = 4
GROUP_DIM = 512
LENGTH = 128
TOKENS = 24576
N_TP = 8


def shard_levels(stream_key, dims, cuts, smallest, high):
    level, own = 1.0, jax.random.fold_in(stream_key, 6)
    for dim, blocks in cuts:
        steps = jnp.exp(jax.random.uniform(jax.random.fold_in(own, dim), (blocks,), jnp.float32, smallest / len(cuts), high / len(cuts)))
        level = level * jnp.repeat(steps, dims[dim] // blocks).reshape([-1 if axis == dim else 1 for axis in range(len(dims))])
    return level


def gaussian(rng, shape, spread, most, shards=(), kind=jnp.bfloat16):
    values = jax.random.normal(rng, shape, jnp.float32) * spread
    if len(shards) > 0:
        values = shard_levels(rng, shape, shards, -0.22, 0.18) * values
    return jnp.clip(values, min=-most, max=most).astype(kind)


def setup_inputs(seed: int = 0) -> dict:
    keys = jax.random.split(jax.random.key(seed), 10)
    tokens = gaussian(keys[0], (TOKENS, D), 1.0, 6.0, ((0, 96),))
    mix_gain = jnp.clip(1.0 + 0.18 * jax.random.normal(keys[1], (D,), jnp.float32), 0.1, 1.9)
    group_weight = gaussian(keys[2], (GROUP_DIM, D), GROUP_DIM ** -0.5, 0.25, ((0, 32), (1, 8)), jnp.float32)
    group_scale = jnp.clip(jnp.exp(math.log(2.0) - 1.3862944 * jax.random.uniform(keys[3], (1, D), jnp.float32) ** shard_levels(keys[3], (1, D), ((1, 8),), -0.2, 0.2)), 0.5, 2.0)
    mlp_gain = jnp.clip(1.0 + 0.18 * jax.random.normal(keys[4], (D,), jnp.float32), 0.1, 1.9)
    up_weight = gaussian(keys[5], (D, FF), D ** -0.5, 0.125, ((0, 32), (1, 8)), jnp.float32)
    up_scale = jnp.clip(jnp.exp(math.log(2.0) - 1.3862944 * jax.random.uniform(keys[6], (1, FF), jnp.float32) ** shard_levels(keys[6], (1, FF), ((1, 8),), -0.2, 0.2)), 0.5, 2.0)
    down_weight = gaussian(keys[7], (FF, D), FF ** -0.5, 0.0625, ((0, 8), (1, 32)), jnp.float32)
    down_scale = jnp.clip(jnp.exp(jax.random.uniform(keys[8], (1, D), jnp.float32, math.log(0.5), math.log(2.0))), 0.5, 2.0)
    return {"tokens": tokens, "mix_gain": mix_gain, "group_weight": group_weight, "group_scale": group_scale, "mlp_gain": mlp_gain, "up_weight": up_weight, "up_scale": up_scale, "down_weight": down_weight, "down_scale": down_scale}


norm_eps = 1e-06

def norm_rows(values, gain):
    promoted = values.astype(jnp.float32)
    inverse = lax.rsqrt(lax.optimization_barrier(jnp.mean(promoted * promoted, axis=-1, keepdims=True)) + norm_eps)
    return (promoted * inverse * gain.astype(jnp.float32)).astype(jnp.bfloat16)

def band_means(inputs, window, seq_length):
    row_count, columns = inputs.shape
    by_sequence = inputs.reshape(row_count // seq_length, seq_length, columns)
    position = jnp.arange(seq_length, dtype=jnp.int32)
    offset = position[:, None] - position[None, :]
    band_mask = ((offset >= 0) & (offset < window)).astype(jnp.float32)
    divisor = jnp.minimum(position + 1, window).astype(jnp.float32)
    summed = jnp.einsum('ts,nsc->ntc', band_mask, by_sequence, precision=lax.Precision.HIGHEST)
    return (summed / divisor[None, :, None] - by_sequence).reshape(row_count, columns)

def reference(tokens, mix_gain, group_weight, group_scale, mlp_gain, up_weight, up_scale, down_weight, down_scale):
    normed = norm_rows(tokens, mix_gain).astype(jnp.float32)
    pieces = []
    for group_index in range(GROUPS):
        first_col = group_index * GROUP_DIM
        inputs = normed[:, first_col:first_col + GROUP_DIM]
        pooled = band_means(inputs, 2 ** (group_index + 1), LENGTH).astype(jnp.bfloat16)
        weight_cols = group_weight[:, first_col:first_col + GROUP_DIM].astype(jnp.bfloat16)
        product = jnp.dot(pooled, weight_cols, preferred_element_type=jnp.float32)
        pieces.append(product * group_scale[:, first_col:first_col + GROUP_DIM])
    mixed_cols = jnp.concatenate(pieces, axis=1)
    carried = (tokens.astype(jnp.float32) + mixed_cols).astype(jnp.bfloat16)
    normed_mlp = norm_rows(carried, mlp_gain)
    pre_act = jnp.dot(normed_mlp, up_weight.astype(jnp.bfloat16), preferred_element_type=jnp.float32) * up_scale
    hidden = jnp.square(jax.nn.relu(pre_act)).astype(jnp.bfloat16)
    tp_block = FF // N_TP
    summed = jnp.zeros(carried.shape, jnp.float32)
    for tp_index in range(N_TP):
        rows_here = slice(tp_index * tp_block, (tp_index + 1) * tp_block)
        partial_value = jnp.dot(hidden[:, rows_here], down_weight[rows_here].astype(jnp.bfloat16), preferred_element_type=jnp.float32) * down_scale
        summed = summed + partial_value.astype(jnp.bfloat16).astype(jnp.float32)
    return (carried.astype(jnp.float32) + summed).astype(jnp.bfloat16)
```

```python
import jax
import jax.numpy as jnp
from jax import lax
from jax.experimental import pallas as pl
from jax.experimental.pallas import tpu as pltpu
from jax.sharding import Mesh
from jax.sharding import PartitionSpec as P

MESH = pl.DeviceIdType.MESH
LENGTH = 128
NY, NZ, NX = 8, 4, 4
CUT = 32
EPS = 1e-06
F32, BF16 = jnp.float32, jnp.bfloat16
SIDES = (1, -1)
AROUND = (1, -1, 2)
SCHEDULE = (
    ("gy",), ("g", 0), ("start", 0), ("zo", 0), ("pool",), ("g", 1), ("g", 7), ("g", 2), ("g", 6), ("g", 3),
    ("g", 5), ("ay", 0, 1, 1), ("ay", 0, 1, -1), ("g", 4), ("zo", 1), ("by1", 0), ("ay", 0, 2, 1),
    ("ay", 0, 2, -1), ("mix",), ("by", 0, 1, 1, 0), ("azs", 0, -1), ("azs", 0, 1), ("azs", 0, -2),
    ("azs", 0, 2), ("by", 0, 1, -1, 0), ("by", 0, 1, 1, 1), ("by", 0, 1, -1, 1), ("ay", 0, 3, 1),
    ("azs", 0, -3), ("ay", 0, 3, -1), ("azs", 0, 3), ("by", 0, 2, 1, 0), ("cz",), ("cx", 0, 1), ("cx", 0, -1),
    ("by", 0, 2, -1, 0), ("by", 0, 2, 1, 1), ("start", 1), ("by", 0, 2, -1, 1), ("ay4", 0), ("azs", 0, 4),
    ("by", 0, 3, 1, 0), ("cx", 0, 2), ("by", 0, 3, -1, 0), ("by", 0, 3, 1, 1), ("by1", 1), ("norm", 0),
    ("ay", 1, 1, -1), ("azs", 1, 1), ("cx", 1, 1), ("cx", 1, -1), ("ay", 1, 1, 1), ("azs", 1, -1),
    ("by", 0, 3, -1, 1), ("by", 1, 1, -1, 0), ("by", 1, 1, 1, 0), ("cx", 1, 2), ("by", 1, 1, -1, 1),
    ("by", 1, 1, 1, 1), ("norm", 1), ("ay", 1, 2, -1), ("azs", 1, 2), ("ay", 1, 2, 1), ("azs", 1, -2),
    ("up",), ("by", 1, 2, 1, 0), ("by", 1, 2, -1, 0), ("comp", 0), ("by", 1, 2, 1, 1), ("by", 1, 2, -1, 1),
    ("ay", 1, 3, 1), ("azs", 1, -3), ("ay", 1, 3, -1), ("azs", 1, 3), ("comp", 1), ("rs1", 0),
    ("by", 1, 3, 1, 0), ("by", 1, 3, -1, 0), ("by", 1, 3, 1, 1), ("rs1", 1), ("by", 1, 3, -1, 1), ("ay4", 1),
    ("azs", 1, 4), ("comp", 2), ("rs2", 0), ("rs1", 2), ("rs2", 1), ("comp", 3), ("ag", 0), ("rs1", 3),
    ("om", 0), ("rs2", 2), ("ag", 1), ("om", 1), ("rs2", 3), ("ag", 2), ("om", 2), ("ag", 3), ("om", 3),
)

def message_keys():
    keys = [("Gy", d) for d in range(1, NY)] + [("Gz", d, e) for d in range(NY) for e in AROUND]
    keys += [("Cz",)] + [("Cx", j, d) for j in (0, 1) for d in AROUND]
    keys += [("Cm", j, d) for j in (0, 1) for d in (0, *AROUND)]
    for w in (0, 1):
        for s in SIDES:
            keys += [("Ay", w, k, s, part) for k in (1, 2, 3, 4) for part in (0, 1)]
            keys += [("By", w, k, s, h) for k in (1, 2, 3) for h in (0, 1)] + [("By", w, 4, s)]
            keys += [("Zo", w, s, n) for n in (1, 2)]
            keys += [("Az", w, o, s, n) for o in (1, -1, 2, -2, 3, -3, 4) for n in (1, 2)]
    for g in range(4):
        keys += [("Pm", g), ("Om", g)] + [("AG", g, d) for d in AROUND]
        keys += [("R", g, 0, d) for d in AROUND] + [("R", g, 1, d) for d in (0, *AROUND)]
    return {key: i for i, key in enumerate(keys)}


KEYS = message_keys()
SOURCES = [(0, d) for d in AROUND] + [(1, d) for d in (0, *AROUND)]


def kernel(
    tokens_hbm, mix_gain, group_hbm, group_scale, mlp_gain, up_hbm, up_scale, down_hbm, down_scale,
    out,
    tokens, group_w, up_w, down_w,
    gw, wu, wd, vu, vd, cx, xs, hidden, part, mate, summed, got, result, scale_at, pooled,
    ssem, rsem, lsem, osem,
):
    rep, z0, y0 = lax.axis_index("rep"), lax.axis_index("z"), lax.axis_index("y")
    x0, c0 = lax.axis_index("x"), lax.axis_index("core")
    tp = x0 * 2 + c0
    q = lax.rem(z0, 2)
    keep, relay = (wu, wd), (vu, vd)
    across = (((1,), (1,)), ((), ()))

    def y_at(d):
        return lax.rem(y0 + (d + NY), NY)

    def z_at(d):
        return lax.rem(z0 + (d + NZ), NZ)

    def x_at(d):
        return lax.rem(x0 + (d + NX), NX)

    def to_y(d):
        return {"y": y_at(d)}

    def to_z(d):
        line = lax.rem(rep * NZ + z0 + (d + 3 * NZ), 3 * NZ)
        return {"rep": lax.div(line, NZ), "z": lax.rem(line, NZ)}

    def to_x(d):
        return {"x": x_at(d)}

    def to_pair(d):
        pair = z0 + 1 - 2 * q
        return {"z": pair} if d == 0 else {"z": pair, "x": x_at(d)}

    to_mate = {"core": 1 - c0}
    sent = []

    def copy(key, ref, dst, device):
        i = KEYS[key]
        return pltpu.make_async_remote_copy(
            src_ref=ref,
            dst_ref=dst,
            send_sem=ssem.at[i],
            recv_sem=rsem.at[i],
            device_id=device,
            device_id_type=MESH,
        )

    def send(key, ref, device, dst=None):
        c = copy(key, ref, ref if dst is None else dst, device)
        c.start()
        sent.append(c)

    def arrived(key, ref):
        copy(key, ref, ref, to_mate).wait_recv()

    def aligned(start, size):
        return pl.ds(pl.multiple_of(start, size), size)

    peers = [to_y(d) for d in range(1, NY)] + [to_z(d) for d in (1, -1, 2, -2)]
    peers += [to_x(d) for d in AROUND] + [to_pair(d) for d in AROUND] + [to_mate]
    barrier = pltpu.get_barrier_semaphore()
    for peer in peers:
        pl.semaphore_signal(barrier, inc=1, device_id=peer, device_id_type=MESH)
    loads = [
        pltpu.make_async_copy(src, dst, lsem.at[i])
        for i, (src, dst) in enumerate(
            [(group_hbm, group_w), (up_hbm, up_w), (down_hbm, down_w), (tokens_hbm, tokens)]
        )
    ]
    for load in loads:
        load.start()

    def shard(w, o, dz, lo=0, hi=64):
        y = y_at(o)
        return keep[w].at[lax.div(y, 2), z_at(dz), lax.rem(y, 2), pl.ds(lo, hi - lo)]

    def b_half(w, o, h):
        y = y_at(o)
        return keep[w].at[lax.div(y, 2), pl.ds(2 * h, 2), lax.rem(y, 2), pl.ds(CUT, 64 - CUT)]

    def passed(w, o, lo=0, hi=64):
        return relay[w].at[y_at(o), pl.ds(lo, hi - lo)]

    def half(s, size, base=0):
        return (base, base + size // 2) if s == 1 else (base + size // 2, base + size)

    step = 1 - 2 * lax.rem(y0, 2)
    m0 = lax.div(y0, 2)
    pair_at = [lax.rem(m0 + d + 4, 4) for d in (0, -step, step, 2)]
    own_half = aligned(c0 * 128, 128)
    mate_half = aligned((1 - c0) * 128, 128)
    my_rows = aligned(c0 * 128 + x0 * 32, 32)

    def cast(w, src):
        mine, other = aligned(q * 512, 512), aligned((1 - q) * 512, 512)
        keep[w][m0, z0, lax.rem(y0, 2)] = src[:, mine].astype(BF16)
        relay[w][y0] = src[:, other].astype(BF16)

    def start(w):
        for s in SIDES:
            send(("Ay", w, 1, s, 0), shard(w, 0, 0, 0, CUT), to_y(s))
            send(("Ay", w, 1, s, 1), passed(w, 0, 0, CUT), to_y(s))

    def zo(w):
        for s in SIDES:
            send(("Zo", w, s, 1), passed(w, 0), to_z(s), shard(w, 0, 0))
        for s in SIDES:
            send(("Zo", w, s, 2), shard(w, 0, 0, *half(s, 64)), to_z(2 * s))

    def by1(w):
        for s in SIDES:
            arrived(("Zo", w, s, 1), shard(w, 0, -s))
            arrived(("Zo", w, s, 2), shard(w, 0, -2 * s, *half(s, 64)))
        for h in (0, 1):
            for s in SIDES:
                send(("By", w, 1, s, h), b_half(w, 0, h), to_y(s))

    def ay(w, k, s):
        arrived(("Ay", w, k, s, 0), shard(w, -s * k, 0, 0, CUT))
        arrived(("Ay", w, k, s, 1), passed(w, -s * k, 0, CUT))
        rows = (0, CUT) if k < 3 else half(s, CUT)
        send(("Ay", w, k + 1, s, 0), shard(w, -s * k, 0, *rows), to_y(s))
        send(("Ay", w, k + 1, s, 1), passed(w, -s * k, *rows), to_y(s))

    def ay4(w):
        for s in SIDES:
            arrived(("Ay", w, 4, s, 0), shard(w, 4, 0, *half(s, CUT)))
            arrived(("Ay", w, 4, s, 1), passed(w, 4, *half(s, CUT)))

    def azs(w, o):
        for s in SIDES:
            send(("Az", w, o, s, 1), passed(w, o, 0, CUT), to_z(s), shard(w, o, 0, 0, CUT))
            send(("Az", w, o, s, 2), shard(w, o, 0, *half(s, CUT)), to_z(2 * s))

    def by(w, k, s, h):
        arrived(("By", w, k, s, h), b_half(w, -s * k, h))
        if k < 3:
            send(("By", w, k + 1, s, h), b_half(w, -s * k, h), to_y(s))
        elif h == (0 if s == 1 else 1):
            send(("By", w, 4, s), b_half(w, -s * k, h), to_y(s))

    def complete(w, *slots):
        for o in slots:
            for s in SIDES:
                arrived(("Az", w, o, s, 1), shard(w, o, -s, 0, CUT))
                arrived(("Az", w, o, s, 2), shard(w, o, -2 * s, *half(s, CUT)))
                if o == 4:
                    arrived(("By", w, 4, s), b_half(w, 4, 0 if s == 1 else 1))

    width = tokens.shape[1]

    def gy():
        loads[0].wait()
        gw[z0, y0] = group_w[...].astype(BF16)
        loads[1].wait()
        cast(0, up_w)
        pl.semaphore_wait(barrier, len(peers))
        for d in (1, 7, 2, 6, 3, 5, 4):
            send(("Gy", d), gw.at[z0, y0], to_y(d))

    def g(d):
        if d:
            arrived(("Gy", d), gw.at[z0, y_at(-d)])
        for e in (1, -1, 2 if d % 2 == 0 else -2):
            send(("Gz", d, abs(e) if abs(e) == 2 else e), gw.at[z0, y_at(-d)], to_z(e))

    def pool():
        loads[2].wait()
        cast(1, down_w)
        loads[3].wait()
        own_group = aligned(x0 * 512, 512)
        whole = tokens[...].astype(F32)
        inverse = lax.rsqrt(jnp.sum(whole * whole, axis=-1, keepdims=True) / width + EPS)
        normed = (tokens[:, own_group].astype(F32) * inverse * mix_gain[:, own_group]).astype(BF16)
        row = lax.broadcasted_iota(jnp.int32, (LENGTH, LENGTH), 0)
        gap = row - lax.broadcasted_iota(jnp.int32, (LENGTH, LENGTH), 1)
        window = jnp.left_shift(jnp.int32(2), x0)
        band = ((gap >= 0) & (gap < window)).astype(F32).astype(BF16)
        position = lax.broadcasted_iota(jnp.int32, (LENGTH, 1), 0)
        divisor = jnp.minimum(position + 1, window).astype(F32)
        for n in range(tokens.shape[0] // LENGTH):
            piece = normed[n * LENGTH : (n + 1) * LENGTH]
            total = jnp.dot(band, piece, preferred_element_type=F32)
            pooled[n * LENGTH : (n + 1) * LENGTH] = (
                total / divisor - piece.astype(F32)
            ).astype(BF16)

    def mix():
        for d in range(NY):
            for e in AROUND:
                back = -e if e != 2 or d % 2 == 0 else 2
                arrived(("Gz", d, e), gw.at[z_at(back), y_at(-d)])
        mixed = jnp.dot(pooled[...], gw[...].reshape(512, 256), preferred_element_type=F32)
        own = tokens[:, aligned(tp * 256, 256)].astype(F32)
        cx[q, tp] = (own + mixed * group_scale[...]).astype(BF16)
        send(("Cz",), cx.at[q, tp], to_pair(0))
        for d in (2, 1, -1):
            send(("Cx", 0, d), cx.at[q, tp], to_x(d))
        send(("Cm", 0, 0), cx.at[q, tp], to_mate)

    def rows_of(j):
        return q if j == 0 else 1 - q

    def cz():
        arrived(("Cz",), cx.at[1 - q, tp])
        for d in (2, 1, -1):
            send(("Cx", 1, d), cx.at[1 - q, tp], to_x(d))
        send(("Cm", 1, 0), cx.at[1 - q, tp], to_mate)

    def cx_(j, d):
        block = cx.at[rows_of(j), x_at(-d) * 2 + c0]
        arrived(("Cx", j, d), block)
        send(("Cm", j, d), block, to_mate)

    def norm(j):
        for d in (0, *AROUND):
            arrived(("Cm", j, d), cx.at[rows_of(j), x_at(-d) * 2 + 1 - c0])
        at = rows_of(j)
        square = None
        for p in range(8):
            v = cx[at, p].astype(F32)
            s = jnp.sum(v * v, axis=-1, keepdims=True)
            square = s if square is None else square + s
        inverse = lax.rsqrt(square / width + EPS)
        for m in range(4):
            for z in range(NZ):
                v = cx[at, 2 * z + m // 2, :, (m % 2) * 128 : (m % 2) * 128 + 128].astype(F32)
                first = z * 512 + m * 128
                xs[m, at, :, z * 128 : z * 128 + 128] = (
                    v * inverse * mlp_gain[:, first : first + 128]
                ).astype(BF16)
        if j == 0:
            for m in range(4):
                for z in range(NZ):
                    first = z * 512 + m * 128
                    scale_at[m, :, z * 128 : z * 128 + 128] = down_scale[:, first : first + 128]

    def up():
        complete(0, 1, -1, 2, -2, 3, -3, 4)

        def tile(n, carry):
            cols = aligned(n * 256, 256)
            acc = None
            for m in range(4):
                t = jnp.dot(
                    xs[m].reshape(512, 512),
                    wu[m, :, :, :, cols].reshape(512, 256),
                    preferred_element_type=F32,
                )
                acc = t if acc is None else acc + t
            acc = jnp.maximum(acc * up_scale[:, aligned(q * 512 + n * 256, 256)], 0.0)
            hidden[:, cols] = (acc * acc).astype(BF16)
            return carry

        lax.fori_loop(0, 2, tile, 0)

    def comp(i):
        complete(1, *((1, -1), (2, -2), (3, -3), (4,))[i])
        m = pair_at[i]
        t = lax.dot_general(
            hidden[...], wd[m].reshape(512, 512), across, preferred_element_type=F32
        )
        part[i] = (t * scale_at[m]).astype(BF16).reshape(2, 256, 512)
        send(("Pm", i), part.at[i, :, mate_half], to_mate, mate.at[i])

    def rs1(i):
        arrived(("Pm", i), mate.at[i])
        summed[i] = (part[i, :, own_half].astype(F32) + mate[i].astype(F32)).astype(BF16)
        for d in (2, 1, -1, 0):
            rows = aligned(x_at(d) * 32, 32)
            place = got.at[i, SOURCES.index((1, d))]
            send(("R", i, 1, d), summed.at[i, 1 - q, rows], to_pair(d), place)
        for d in (2, 1, -1):
            rows = aligned(x_at(d) * 32, 32)
            place = got.at[i, SOURCES.index((0, d))]
            send(("R", i, 0, d), summed.at[i, q, rows], to_x(d), place)

    def rs2(i):
        m = pair_at[i]
        total = summed[i, q, aligned(x0 * 32, 32)].astype(F32)
        for n, (side, d) in enumerate(SOURCES):
            arrived(("R", i, side, d), got.at[i, n])
            total = total + got[i, n].astype(F32)
        for z in range(NZ):
            base = cx[q, 2 * z + lax.div(m, 2), my_rows, aligned(lax.rem(m, 2) * 128, 128)]
            lanes = slice(z * 128, z * 128 + 128)
            result[m, my_rows, lanes] = (base.astype(F32) + total[:, lanes]).astype(BF16)
        for d in (2, 1, -1):
            send(("AG", i, d), result.at[m, my_rows], to_x(d))

    def ag(i):
        m = pair_at[i]
        for d in AROUND:
            rows = aligned(c0 * 128 + x_at(-d) * 32, 32)
            arrived(("AG", i, d), result.at[m, rows])
        send(("Om", i), result.at[m, own_half], to_mate)

    stores = []

    def om(i):
        m = pair_at[i]
        arrived(("Om", i), result.at[m, mate_half])
        for z in range(NZ):
            c = pltpu.make_async_copy(
                result.at[m, :, pl.ds(z * 128, 128)],
                out.at[:, aligned(z * 512 + m * 128, 128)],
                osem.at[i, z],
            )
            c.start()
            stores.append(c)

    tasks = dict(
        gy=gy, g=g, start=start, zo=zo, by1=by1, ay=ay, ay4=ay4, azs=azs, by=by, pool=pool, mix=mix,
        cz=cz, cx=cx_, norm=norm, up=up, comp=comp, rs1=rs1, rs2=rs2, ag=ag, om=om,
    )
    for name, *where in SCHEDULE:
        with jax.named_scope("_".join([name, *(str(v) for v in where)])):
            tasks[name](*where)
    with jax.named_scope("stores"):
        for c in stores:
            c.wait()
    with jax.named_scope("sent"):
        for c in sent:
            c.wait_send()


def body(tokens, mix_gain, group_w, group_scale, mlp_gain, up_w, up_scale, down_w, down_scale):
    rows, width = tokens.shape
    n = len(KEYS)
    vmem, hbm = pl.BlockSpec(memory_space=pltpu.VMEM), pl.BlockSpec(memory_space=pl.ANY)
    shard_shape = up_w.shape
    return pl.pallas_call(
        kernel,
        name="layer",
        out_shape=jax.ShapeDtypeStruct((rows, width), BF16),
        in_specs=[hbm, vmem, hbm, vmem, vmem, hbm, vmem, hbm, vmem],
        out_specs=hbm,
        scratch_shapes=[
            pltpu.VMEM((rows, width), BF16),
            pltpu.VMEM(group_w.shape, F32),
            pltpu.VMEM(shard_shape, F32),
            pltpu.VMEM(shard_shape, F32),
            pltpu.VMEM((NZ, NY, 16, 256), BF16),
            pltpu.VMEM((4, NZ, 2, 64, 512), BF16),
            pltpu.VMEM((4, NZ, 2, 64, 512), BF16),
            pltpu.VMEM((NY, 64, 512), BF16),
            pltpu.VMEM((NY, 64, 512), BF16),
            pltpu.VMEM((2, 8, rows, 256), BF16),
            pltpu.VMEM((4, 2, rows, 512), BF16),
            pltpu.VMEM((2 * rows, 512), BF16),
            pltpu.VMEM((4, 2, rows, 512), BF16),
            pltpu.VMEM((4, 2, rows // 2, 512), BF16),
            pltpu.VMEM((4, 2, rows // 2, 512), BF16),
            pltpu.VMEM((4, len(SOURCES), 32, 512), BF16),
            pltpu.VMEM((4, rows, 512), BF16),
            pltpu.VMEM((4, 1, 512), F32),
            pltpu.VMEM((rows, 512), BF16),
            pltpu.SemaphoreType.DMA((n,)),
            pltpu.SemaphoreType.DMA((n,)),
            pltpu.SemaphoreType.DMA((4,)),
            pltpu.SemaphoreType.DMA((4, NZ)),
        ],
        compiler_params=pltpu.CompilerParams(
            collective_id=0, has_side_effects=True, vmem_limit_bytes=56 * 1024 * 1024
        ),
    )(
        tokens,
        mix_gain.reshape(1, width),
        group_w,
        group_scale,
        mlp_gain.reshape(1, width),
        up_w,
        up_scale,
        down_w.T,
        down_scale,
    )


def solution(mesh):
    split = Mesh(
        mesh.devices.reshape(mesh.shape["rep"], NZ, NY, NX, 2), ("rep", "z", "y", "x", "core")
    )
    fs, tp = ("z", "y"), ("x", "core")
    rows = P(("rep", "z", "y"), None)
    return jax.shard_map(
        body,
        mesh=split,
        in_specs=(
            rows,
            P(),
            P(fs, tp),
            P(None, tp),
            P(),
            P(fs, tp),
            P(None, tp),
            P(tp, fs),
            P(),
        ),
        out_specs=rows,
        check_vma=False,
    )
```
